32 devices in a mesh: ep: 8 (over z, x), tp: 4 (over y, core).
Axes of the slice: x: 2, y: 2, z: 4, core: 2. Of those that a mesh axis runs over, the one named last changes fastest.
Arguments:
- tokens: bfloat16 [384, 1024], P('ep'), may hold values from -6 to 6
- head_state: float32 [384, 8, 64, 64], P('ep', 'tp'), may hold values from -6 to 6
- recept_weight: bfloat16 [1024, 512], P(None, 'tp'), may hold values from -0.1875 to 0.1875
- key_weight: bfloat16 [1024, 512], P(None, 'tp'), may hold values from -0.1875 to 0.1875
- value_weight: bfloat16 [1024, 512], P(None, 'tp'), may hold values from -0.1875 to 0.1875
- decay_down_factor: bfloat16 [1024, 64], replicated, may hold values from -0.1875 to 0.1875
- decay_up_factor: bfloat16 [64, 512], P(None, 'tp'), may hold values from -0.75 to 0.75
- decay_base: float32 [512], P('tp'), may hold values from -5 to 3
- rate_down_factor: bfloat16 [1024, 64], replicated, may hold values from -0.1875 to 0.1875
- rate_up_factor: bfloat16 [64, 512], P(None, 'tp'), may hold values from -0.75 to 0.75
- rate_base: float32 [512], P('tp'), may hold values from -3 to 3
- head_gain: float32 [512], P('tp'), may hold values from 0.1 to 1.9
- out_weight: bfloat16 [512, 1024], P('tp'), may hold values from -0.25 to 0.25
- route_experts: int32 [384, 4], P('ep'), may hold values from 0 to 7, all different within a row; in each aligned block of 48 rows (0 to 47, 48 to 95, ...) at most 48 rows name the same one
- route_weights: float32 [384, 4], P('ep'), may hold values from 0.03 to 0.2
- expert_gate: bfloat16 [8, 1024, 1024], P('ep', None, 'tp'), may hold values from -1 to 1
- expert_up: bfloat16 [8, 1024, 1024], P('ep', None, 'tp'), may hold values from -1 to 1
- expert_down: bfloat16 [8, 1024, 1024], P('ep', 'tp'), may hold values from -0.1875 to 0.1875
Outputs:
- layer_out: bfloat16 [384, 1024], P('ep', 'tp')
- new_state: float32 [384, 8, 64, 64], P('ep', 'tp')
The draws below stay inside these ranges and needn't reach their ends.
Inputs may be any that keep to these rules, and one draw needn't show every extreme that they name: `route_experts`: each row names 4 different experts. In each aligned block of 48 rows no expert is named by more than 48 rows, a bound that some block reaches.
All inputs are finite; a program needn't handle non-finite values.
Results may differ from the reference program's by a relative error of at most 0.02.
Values may be sent and summed in bfloat16 or wider, within the bound.
No kernel may reach another device: no remote copies, remote signals or barrier semaphores. Data moves between devices by JAX's collectives and lax.ppermute only.
A program may use at most 128 MiB of HBM per device.

```python
import math
import jax
import jax.numpy as jnp
import numpy as np
from jax import lax

MODEL_DIMENSION = 1024
ALL_HEADS_WIDTH = 512
HEAD_DIM = 64
HEADS = 8
LOW_RANK_WIDTH = 64
DE = 1024
TOP_K = 4
SEQ_DEV = 48
SEQS = 384
EXPERTS = 8
CAP = 48
N_EP = 8
N_TP = 4


def column_scaled(key, stream):
    folded = jax.random.fold_in(key, stream)
    entries = jax.random.truncated_normal(jax.random.fold_in(folded, 1), -6.0, 6.0, (EXPERTS, MODEL_DIMENSION, DE), jnp.float32)
    column_scale = jnp.exp(jax.random.uniform(jax.random.fold_in(folded, 2), (EXPERTS, 1, DE), jnp.float32) * math.log(8.0))
    return jnp.clip(entries * column_scale / math.sqrt(MODEL_DIMENSION), -1.0, 1.0).astype(jnp.bfloat16)


def draw_expert_gate(key, part):
    return column_scaled(key, 11)


def draw_expert_up(key, part):
    return column_scaled(key, 23)


def block_levels(rng, shape, pieces, smallest, high):
    loudness, own = 1.0, jax.random.fold_in(rng, 6)
    for position, shards_of in pieces:
        heights = jnp.exp(jax.random.uniform(jax.random.fold_in(own, position), (shards_of,), jnp.float32, smallest / len(pieces), high / len(pieces)))
        loudness = loudness * jnp.repeat(heights, shape[position] // shards_of).reshape([-1 if axis == position else 1 for axis in range(len(shape))])
    return loudness


def shared_out(key, own, number, rows, count, top, bound, lean):
    sequence = jax.random.permutation(key, count)
    crowded, usual = load_shares(count, rows * top, bound, lean, True), load_shares(count, rows * top, bound, lean, False)
    places = jnp.arange(count)

    def named(sizes, offset_by):
        used = int((sizes > 0).sum())
        fixed = max(1, used // 4)
        moved = fixed + (places - fixed + offset_by * (used - fixed)) % max(1, count - fixed)
        return jnp.zeros((count,), jnp.int32).at[sequence[jnp.where(places < fixed, places, moved)]].set(jnp.asarray(sizes, jnp.int32))

    sizes = jnp.where(number % 4 == 0, named(crowded, number // 4), named(usual, number - number // 4 - 1))
    mixed = jax.random.permutation(jax.random.fold_in(own, 3), count)
    source_of, sink = mixed[0:count // 2 * 2:2], mixed[1:count // 2 * 2:2]
    slack = jnp.minimum(sizes[source_of] - 1, bound - sizes[sink]) // 2
    slack = jnp.where((source_of == sequence[0]) | (sink == sequence[0]) | (sizes[sink] == 0), 0, jnp.maximum(slack, 0))
    moved = jax.random.randint(jax.random.fold_in(own, 4), (count // 2,), 0, 1 << 20) % (slack + 1)
    sizes = sizes.at[source_of].add(-moved).at[sink].add(moved)
    labels = jnp.searchsorted(jnp.cumsum(sizes), jnp.arange(rows * top), side="right").astype(jnp.int32)
    grid = labels.reshape(top, rows).T
    grid = grid[jax.random.permutation(jax.random.fold_in(own, 1), rows)]
    offset_by = jax.random.randint(jax.random.fold_in(own, 2), (rows, 1), 0, top)
    return jnp.take_along_axis(grid, (jnp.arange(top)[None, :] + offset_by) % top, axis=1)


def load_shares(number_of, total, most, lean, full):
    weights = [(1 << 20) // math.isqrt(grade ** lean) + 1 for grade in range(1, number_of + 1)]
    largest = most if full else min(most, max(-(-total // number_of), total * weights[0] // sum(weights)))
    least = 1 if total - largest >= number_of - 1 else 0
    counts, rest = [largest] + [least] * (number_of - 1), total - largest - least * (number_of - 1)
    while rest > 0:
        movable = [i for i in range(1, number_of) if counts[i] < largest] or [i for i in range(1, number_of) if counts[i] < most]
        mass, budget = sum([weights[i] for i in movable]), rest
        for i in movable:
            addition = min(most - counts[i], max(1, budget * weights[i] // mass), rest)
            counts[i] = counts[i] + addition
            rest = rest - addition
    return np.array(counts)


def gaussian(own_key, dims, scale, bound, cuts=(), kind=jnp.bfloat16):
    result = jax.random.normal(own_key, dims, jnp.float32) * scale
    if len(cuts) > 0:
        result = block_levels(own_key, dims, cuts, -0.22, 0.18) * result
    return jnp.clip(result, min=-bound, max=bound).astype(kind)


def setup_inputs(seed: int = 0) -> dict:
    arg_keys = jax.random.split(jax.random.key(seed), 19)
    tokens = gaussian(arg_keys[0], (SEQS, MODEL_DIMENSION), 1.0, 6.0, ((0, 8),))
    head_state = gaussian(arg_keys[1], (SEQS, HEADS, HEAD_DIM, HEAD_DIM), 1.0, 6.0, ((0, 8), (1, 4)), jnp.float32)
    recept_weight = gaussian(arg_keys[2], (MODEL_DIMENSION, ALL_HEADS_WIDTH), MODEL_DIMENSION ** -0.5, 0.1875, ((1, 4),))
    key_weight = gaussian(arg_keys[3], (MODEL_DIMENSION, ALL_HEADS_WIDTH), MODEL_DIMENSION ** -0.5, 0.1875, ((1, 4),))
    value_weight = gaussian(arg_keys[4], (MODEL_DIMENSION, ALL_HEADS_WIDTH), MODEL_DIMENSION ** -0.5, 0.1875, ((1, 4),))
    decay_down_factor = gaussian(arg_keys[5], (MODEL_DIMENSION, LOW_RANK_WIDTH), MODEL_DIMENSION ** -0.5, 0.1875)
    decay_up_factor = gaussian(arg_keys[6], (LOW_RANK_WIDTH, ALL_HEADS_WIDTH), LOW_RANK_WIDTH ** -0.5, 0.75, ((1, 4),))
    decay_base = jnp.clip(-5.0 + 8.0 * jax.random.uniform(arg_keys[7], (ALL_HEADS_WIDTH,), jnp.float32) ** block_levels(arg_keys[7], (ALL_HEADS_WIDTH,), ((0, 4),), -0.2, 0.2), -5.0, 3.0)
    rate_down_factor = gaussian(arg_keys[8], (MODEL_DIMENSION, LOW_RANK_WIDTH), MODEL_DIMENSION ** -0.5, 0.1875)
    rate_up_factor = gaussian(arg_keys[9], (LOW_RANK_WIDTH, ALL_HEADS_WIDTH), LOW_RANK_WIDTH ** -0.5, 0.75, ((1, 4),))
    rate_base = jnp.clip(jax.random.uniform(arg_keys[10], (ALL_HEADS_WIDTH,), jnp.float32, -3.0, 3.0) * block_levels(arg_keys[10], (ALL_HEADS_WIDTH,), ((0, 4),), -0.4, 0.0), -3.0, 3.0)
    head_gain = jnp.clip(1.0 + 0.18 * jax.random.normal(arg_keys[11], (ALL_HEADS_WIDTH,), jnp.float32), 0.1, 1.9)
    out_weight = gaussian(arg_keys[12], (ALL_HEADS_WIDTH, MODEL_DIMENSION), ALL_HEADS_WIDTH ** -0.5, 0.25, ((0, 4),))
    route_experts_keys = jax.random.split(jax.random.fold_in(arg_keys[13], 1), SEQS // SEQ_DEV)
    route_experts_turns = jax.random.permutation(jax.random.fold_in(arg_keys[13], 3), SEQS // SEQ_DEV)
    route_experts = jax.vmap(lambda own, number: shared_out(jax.random.fold_in(arg_keys[13], 2), own, number, SEQ_DEV, EXPERTS, TOP_K, CAP, 2))(route_experts_keys, route_experts_turns).reshape((SEQS, TOP_K))
    route_weights = jnp.clip(jnp.exp(math.log(0.2) - 1.89712 * jax.random.uniform(arg_keys[14], (SEQS, TOP_K), jnp.float32) ** block_levels(arg_keys[14], (SEQS, TOP_K), ((0, 8),), -0.2, 0.2)), 0.03, 0.2)
    expert_gate = draw_expert_gate(jax.random.fold_in(arg_keys[18], 71), 0)
    expert_up = draw_expert_up(jax.random.fold_in(arg_keys[18], 71), 0)
    expert_down = gaussian(arg_keys[17], (EXPERTS, DE, MODEL_DIMENSION), DE ** -0.5, 0.1875, ((0, 8), (1, 4)))
    return dict(tokens=tokens, head_state=head_state, recept_weight=recept_weight, key_weight=key_weight, value_weight=value_weight, decay_down_factor=decay_down_factor, decay_up_factor=decay_up_factor, decay_base=decay_base, rate_down_factor=rate_down_factor, rate_up_factor=rate_up_factor, rate_base=rate_base, head_gain=head_gain, out_weight=out_weight, route_experts=route_experts, route_weights=route_weights, expert_gate=expert_gate, expert_up=expert_up, expert_down=expert_down)


NORM_EPS = 1e-05
GROUP_EPS = 0.00064
UNIT_EPS = 1e-06
CLAMP_LIMIT = 7.0
GLU_ALPHA = 1.702

def row_norm(values):
    return values * lax.rsqrt(lax.optimization_barrier(jnp.mean(values * values, axis=-1, keepdims=True)) + NORM_EPS)

def clamped_unit(gate_pre, up_pre):
    gated = jnp.minimum(gate_pre, CLAMP_LIMIT)
    linear = jnp.clip(up_pre, -CLAMP_LIMIT, CLAMP_LIMIT)
    return gated * jax.nn.sigmoid(GLU_ALPHA * gated) * (linear + 1.0)

def update_heads(head_state, recept, keys, values, decay_rate, rate_gate, head_gain):
    seq_count, head_count, head_size = head_state.shape[:3]

    def by_heads(operand):
        return operand.astype(jnp.float32).reshape(seq_count, head_count, head_size)
    recept_heads = by_heads(recept)
    key_heads = by_heads(keys)
    value_heads = by_heads(values)
    decay_heads = by_heads(decay_rate)
    rate_heads = by_heads(rate_gate)
    unit_key = key_heads * lax.rsqrt(lax.optimization_barrier(jnp.sum(key_heads * key_heads, axis=-1, keepdims=True)) + UNIT_EPS)
    highest = lax.Precision.HIGHEST
    state_unit = jnp.einsum('shvk,shk->shv', head_state, unit_key, precision=highest)
    new_state = head_state * decay_heads[:, :, None, :] - state_unit[..., None] * (unit_key * rate_heads)[:, :, None, :] + value_heads[..., None] * (key_heads * rate_heads)[:, :, None, :]
    head_out = jnp.einsum('shvk,shk->shv', new_state, recept_heads, precision=highest)
    centre = lax.optimization_barrier(jnp.mean(head_out, axis=-1, keepdims=True))
    spread = lax.optimization_barrier(jnp.mean(jnp.square(head_out - centre), axis=-1, keepdims=True))
    normed_heads = (head_out - centre) * lax.rsqrt(spread + GROUP_EPS)
    mixed = (normed_heads.reshape(seq_count, -1) * head_gain).astype(jnp.bfloat16)
    return (new_state, mixed)

def reference(tokens, head_state, recept_weight, key_weight, value_weight, decay_down_factor, decay_up_factor, decay_base, rate_down_factor, rate_up_factor, rate_base, head_gain, out_weight, route_experts, route_weights, expert_gate, expert_up, expert_down):
    tokens_float = tokens.astype(jnp.float32)
    normed = row_norm(tokens_float).astype(jnp.bfloat16)
    recept = jnp.dot(normed, recept_weight, preferred_element_type=jnp.float32).astype(jnp.bfloat16)
    keys = jnp.dot(normed, key_weight, preferred_element_type=jnp.float32).astype(jnp.bfloat16)
    values = jnp.dot(normed, value_weight, preferred_element_type=jnp.float32).astype(jnp.bfloat16)
    decay_low = jnp.tanh(jnp.dot(normed, decay_down_factor, preferred_element_type=jnp.float32)).astype(jnp.bfloat16)
    rate_low = jnp.dot(normed, rate_down_factor, preferred_element_type=jnp.float32).astype(jnp.bfloat16)
    decay_pre = decay_base + jnp.dot(decay_low, decay_up_factor, preferred_element_type=jnp.float32)
    decay_rate = jnp.exp(-jnp.exp(-jax.nn.softplus(-decay_pre) - 0.5))
    rate_gate = jax.nn.sigmoid(rate_base + jnp.dot(rate_low, rate_up_factor, preferred_element_type=jnp.float32))
    new_state, mixed = update_heads(head_state, recept, keys, values, decay_rate, rate_gate, head_gain)
    group_width = ALL_HEADS_WIDTH // N_TP
    partials = jnp.einsum('sgr,grd->gsd', mixed.reshape(SEQS, N_TP, group_width).astype(jnp.float32), out_weight.reshape(N_TP, group_width, MODEL_DIMENSION).astype(jnp.float32))
    partials = lax.optimization_barrier(partials.astype(jnp.bfloat16)).astype(jnp.float32)
    residual = (tokens_float + lax.optimization_barrier(jnp.sum(partials, axis=0))).astype(jnp.bfloat16)
    expert_input = row_norm(residual.astype(jnp.float32)).astype(jnp.bfloat16)
    grouped = route_experts.reshape(N_EP, SEQ_DEV * TOP_K)
    onehot = (grouped[:, :, None] == jnp.arange(EXPERTS, dtype=jnp.int32)[None, None, :]).astype(jnp.int32)
    earlier = jnp.cumsum(onehot, axis=1) - onehot
    slot_rank = lax.optimization_barrier(jnp.sum(earlier * onehot, axis=-1)).astype(jnp.int32)
    target = (grouped * CAP + slot_rank).astype(jnp.int32)
    repeated = jnp.repeat(expert_input.reshape(N_EP, SEQ_DEV, MODEL_DIMENSION), TOP_K, axis=1)
    sources = jnp.arange(N_EP, dtype=jnp.int32)[:, None]
    buffer = jnp.zeros((N_EP, EXPERTS * CAP, MODEL_DIMENSION), jnp.bfloat16).at[sources, target].set(repeated)
    per_expert = buffer.reshape(N_EP, EXPERTS, CAP, MODEL_DIMENSION).transpose(1, 0, 2, 3).reshape(EXPERTS, N_EP * CAP, MODEL_DIMENSION)
    hidden_group = DE // N_TP

    def one_expert(operands):
        slot_rows, gate_matrix, up_matrix, down_matrix = operands
        gate_pre = jnp.dot(slot_rows, gate_matrix, preferred_element_type=jnp.float32)
        up_pre = jnp.dot(slot_rows, up_matrix, preferred_element_type=jnp.float32)
        activated = clamped_unit(gate_pre, up_pre).astype(jnp.bfloat16)
        expert_parts = jnp.einsum('rgc,gcd->grd', activated.reshape(-1, N_TP, hidden_group).astype(jnp.float32), down_matrix.reshape(N_TP, hidden_group, MODEL_DIMENSION).astype(jnp.float32))
        expert_parts = lax.optimization_barrier(expert_parts.astype(jnp.bfloat16)).astype(jnp.float32)
        return lax.optimization_barrier(jnp.sum(expert_parts, axis=0)).astype(jnp.bfloat16)
    results = lax.map(one_expert, (per_expert, expert_gate, expert_up, expert_down))
    returned = results.reshape(EXPERTS, N_EP, CAP, MODEL_DIMENSION).transpose(1, 0, 2, 3).reshape(N_EP, EXPERTS * CAP, MODEL_DIMENSION)
    picked = jnp.take_along_axis(returned, target[:, :, None], axis=1)
    picked = picked.reshape(SEQS, TOP_K, MODEL_DIMENSION).astype(jnp.float32)
    mixture = lax.optimization_barrier(jnp.sum(route_weights[:, :, None] * picked, axis=1))
    layer_out = (residual.astype(jnp.float32) + mixture).astype(jnp.bfloat16)
    return (layer_out, new_state)
```

```python
import jax
import jax.numpy as jnp
from jax import lax
from jax.sharding import PartitionSpec as P

NORM_EPS = 1e-05
GROUP_EPS = 0.00064
UNIT_EPS = 1e-06
CLAMP_LIMIT = 7.0
GLU_ALPHA = 1.702


def row_norm(values):
    return values * lax.rsqrt(jnp.mean(values * values, axis=-1, keepdims=True) + NORM_EPS)


def clamped_unit(gate_pre, up_pre):
    gated = jnp.minimum(gate_pre, CLAMP_LIMIT)
    linear = jnp.clip(up_pre, -CLAMP_LIMIT, CLAMP_LIMIT)
    return gated * jax.nn.sigmoid(GLU_ALPHA * gated) * (linear + 1.0)


def update_heads(head_state, recept, keys, values, decay_rate, rate_gate, head_gain):
    seq_count, head_count, head_size = head_state.shape[:3]

    def by_heads(operand):
        return operand.astype(jnp.float32).reshape(seq_count, head_count, head_size)

    recept_heads = by_heads(recept)
    key_heads = by_heads(keys)
    value_heads = by_heads(values)
    decay_heads = by_heads(decay_rate)
    rate_heads = by_heads(rate_gate)
    unit_key = key_heads * lax.rsqrt(
        jnp.sum(key_heads * key_heads, axis=-1, keepdims=True) + UNIT_EPS
    )
    highest = lax.Precision.HIGHEST
    state_unit = jnp.einsum("shvk,shk->shv", head_state, unit_key, precision=highest)
    new_state = (
        head_state * decay_heads[:, :, None, :]
        - state_unit[..., None] * (unit_key * rate_heads)[:, :, None, :]
        + value_heads[..., None] * (key_heads * rate_heads)[:, :, None, :]
    )
    head_out = jnp.einsum("shvk,shk->shv", new_state, recept_heads, precision=highest)
    centre = jnp.mean(head_out, axis=-1, keepdims=True)
    spread = jnp.mean(jnp.square(head_out - centre), axis=-1, keepdims=True)
    normed_heads = (head_out - centre) * lax.rsqrt(spread + GROUP_EPS)
    mixed = (normed_heads.reshape(seq_count, -1) * head_gain).astype(jnp.bfloat16)
    return (new_state, mixed)


def attention(
    tokens,
    head_state,
    recept_weight,
    key_weight,
    value_weight,
    decay_down_factor,
    decay_up_factor,
    decay_base,
    rate_down_factor,
    rate_up_factor,
    rate_base,
    head_gain,
):
    tokens_float = tokens.astype(jnp.float32)
    normed = row_norm(tokens_float).astype(jnp.bfloat16)
    recept = jnp.dot(normed, recept_weight, preferred_element_type=jnp.float32).astype(jnp.bfloat16)
    keys = jnp.dot(normed, key_weight, preferred_element_type=jnp.float32).astype(jnp.bfloat16)
    values = jnp.dot(normed, value_weight, preferred_element_type=jnp.float32).astype(jnp.bfloat16)
    decay_low = jnp.tanh(
        jnp.dot(normed, decay_down_factor, preferred_element_type=jnp.float32)
    ).astype(jnp.bfloat16)
    rate_low = jnp.dot(normed, rate_down_factor, preferred_element_type=jnp.float32).astype(
        jnp.bfloat16
    )
    decay_pre = decay_base + jnp.dot(decay_low, decay_up_factor, preferred_element_type=jnp.float32)
    decay_rate = jnp.exp(-jnp.exp(-jax.nn.softplus(-decay_pre) - 0.5))
    rate_gate = jax.nn.sigmoid(
        rate_base + jnp.dot(rate_low, rate_up_factor, preferred_element_type=jnp.float32)
    )
    new_state, mixed = update_heads(
        head_state, recept, keys, values, decay_rate, rate_gate, head_gain
    )
    return (new_state, mixed)


def compact_local(
    tokens,
    head_state,
    recept_weight,
    key_weight,
    value_weight,
    decay_down_factor,
    decay_up_factor,
    decay_base,
    rate_down_factor,
    rate_up_factor,
    rate_base,
    head_gain,
    out_weight,
    route_experts,
    route_weights,
    expert_gate,
    expert_up,
    expert_down,
):
    tokens_float = tokens.astype(jnp.float32)
    new_state, mixed = attention(
        tokens,
        head_state,
        recept_weight,
        key_weight,
        value_weight,
        decay_down_factor,
        decay_up_factor,
        decay_base,
        rate_down_factor,
        rate_up_factor,
        rate_base,
        head_gain,
    )
    partial_value = jnp.dot(mixed, out_weight, preferred_element_type=jnp.float32).astype(
        jnp.bfloat16
    )
    partial_value = lax.optimization_barrier(partial_value).astype(jnp.float32)
    summed = lax.psum(partial_value.astype(jnp.bfloat16), "tp").astype(jnp.float32)
    residual = (tokens_float + summed).astype(jnp.bfloat16)
    expert_input = row_norm(residual.astype(jnp.float32)).astype(jnp.bfloat16)
    seq_count, top_count = route_experts.shape
    expert_count = lax.axis_size("ep")
    capacity = max(2, (2 * seq_count * top_count + expert_count - 1) // expert_count)
    column_count = expert_input.shape[1] // lax.axis_size("tp")
    column_start = lax.axis_index("tp") * column_count
    flat_routes = route_experts.reshape(-1)
    onehot = (flat_routes[:, None] == jnp.arange(expert_count, dtype=jnp.int32)[None, :]).astype(
        jnp.int32
    )
    earlier = jnp.cumsum(onehot, axis=0) - onehot
    target = flat_routes * capacity + jnp.sum(earlier * onehot, axis=1)
    slot_ids = jnp.arange(expert_count * capacity, dtype=jnp.int32)
    dispatch_map = jnp.any(
        slot_ids[:, None, None] == target.reshape(seq_count, top_count)[None], axis=-1
    )
    dispatch_map = dispatch_map.astype(jnp.bfloat16)
    outgoing = lax.dynamic_slice_in_dim(expert_input, column_start, column_count, 1)
    buffer = jnp.dot(dispatch_map, outgoing, preferred_element_type=jnp.float32).astype(
        jnp.bfloat16
    )
    buffer = buffer.reshape(expert_count, capacity, outgoing.shape[1])
    slot_rows = lax.all_gather(
        lax.all_to_all(buffer, "ep", split_axis=0, concat_axis=0, tiled=True),
        "tp",
        axis=2,
        tiled=True,
    )
    source_count, slot_count, model_width = slot_rows.shape
    flat_rows = slot_rows.reshape(-1, model_width)
    gate_pre = jnp.dot(flat_rows, expert_gate[0], preferred_element_type=jnp.float32)
    up_pre = jnp.dot(flat_rows, expert_up[0], preferred_element_type=jnp.float32)
    activated = clamped_unit(gate_pre, up_pre).astype(jnp.bfloat16)
    part_out = jnp.dot(activated, expert_down[0], preferred_element_type=jnp.float32).astype(
        jnp.bfloat16
    )
    part_out = lax.optimization_barrier(part_out).astype(jnp.float32)
    part_out = part_out.reshape(source_count, slot_count, model_width)
    shares = lax.psum_scatter(part_out.astype(jnp.bfloat16), "tp", scatter_dimension=2, tiled=True)
    returned = lax.all_to_all(shares, "ep", split_axis=0, concat_axis=0, tiled=True)
    picked = returned.reshape(expert_count * capacity, column_count)[target]
    picked = picked.reshape(seq_count, top_count, column_count).astype(jnp.float32)
    mixture = jnp.sum(route_weights[:, :, None] * picked, axis=1)
    own_residual = lax.dynamic_slice_in_dim(residual, column_start, column_count, 1).astype(
        jnp.float32
    )
    layer_out = (own_residual + mixture).astype(jnp.bfloat16)
    return (layer_out, new_state)


def swap(operand, axis, offset):
    size = lax.axis_size(axis)
    return lax.ppermute(operand, axis, [(i, i ^ offset) for i in range(size)])


def swap_both(operand, ep_offset, tp_offset):
    ep_size, tp_size = lax.axis_size("ep"), lax.axis_size("tp")
    pairs = [
        (e * tp_size + t, (e ^ ep_offset) * tp_size + (t ^ tp_offset))
        for e in range(ep_size)
        for t in range(tp_size)
    ]
    return lax.ppermute(operand, ("ep", "tp"), pairs)


def dense_local(
    tokens,
    head_state,
    recept_weight,
    key_weight,
    value_weight,
    decay_down_factor,
    decay_up_factor,
    decay_base,
    rate_down_factor,
    rate_up_factor,
    rate_base,
    head_gain,
    out_weight,
    route_experts,
    route_weights,
    expert_gate,
    expert_up,
    expert_down,
):
    ep_size, tp_size = lax.axis_size("ep"), lax.axis_size("tp")
    ep_index, tp_index = lax.axis_index("ep"), lax.axis_index("tp")
    seq_count, model_width = tokens.shape
    half = model_width // 2
    quarter = model_width // tp_size
    odd = tp_index % 2 == 1

    own_half = jnp.where(odd, tokens[:, half:], tokens[:, :half])
    other_tokens = jnp.concatenate([swap(own_half, "ep", k) for k in range(1, ep_size)], axis=0)
    weight_far = swap(out_weight, "tp", 2)
    weight_pair = jnp.concatenate([out_weight, weight_far], axis=0)
    weight_all = jnp.concatenate([weight_pair, swap(weight_pair, "tp", 1)], axis=0)
    partner_tokens = swap(other_tokens, "tp", 1)
    low = jnp.where(odd, partner_tokens, other_tokens)
    high = jnp.where(odd, other_tokens, partner_tokens)
    tokens_all = jnp.concatenate([tokens, jnp.concatenate([low, high], axis=1)], axis=0)

    new_state, mixed = attention(
        tokens,
        head_state,
        recept_weight,
        key_weight,
        value_weight,
        decay_down_factor,
        decay_up_factor,
        decay_base,
        rate_down_factor,
        rate_up_factor,
        rate_base,
        head_gain,
    )

    near = [mixed] + [swap_both(mixed, k, 0) for k in range(1, ep_size)]
    far = [swap_both(mixed, k, 2) for k in range(ep_size)]
    mixed_pair = jnp.concatenate(
        [jnp.concatenate(near, axis=0), jnp.concatenate(far, axis=0)], axis=1
    )
    mixed_all = jnp.concatenate([mixed_pair, swap(mixed_pair, "tp", 1)], axis=1)
    projected = jnp.dot(mixed_all, weight_all, preferred_element_type=jnp.float32)
    residual = (tokens_all.astype(jnp.float32) + projected).astype(jnp.bfloat16)
    expert_input = row_norm(residual.astype(jnp.float32)).astype(jnp.bfloat16)

    gate_pre = jnp.dot(expert_input, expert_gate[0], preferred_element_type=jnp.float32)
    up_pre = jnp.dot(expert_input, expert_up[0], preferred_element_type=jnp.float32)
    activated = clamped_unit(gate_pre, up_pre).astype(jnp.bfloat16)

    def down(slots):
        pieces = [
            lax.dynamic_slice_in_dim(expert_down[0], (tp_index ^ j) * quarter, quarter, 1)
            for j in slots
        ]
        return jnp.dot(
            activated, jnp.concatenate(pieces, axis=1), preferred_element_type=jnp.float32
        )

    sent = down((1, 3)).astype(jnp.bfloat16)
    kept = down((0, 2))
    pair_sum = (kept + swap(sent, "tp", 1).astype(jnp.float32)).astype(jnp.bfloat16)
    pair_sum = pair_sum.reshape(ep_size, seq_count, 2 * quarter)
    slots = jnp.arange(ep_size, dtype=jnp.int32) ^ ep_index
    hits = route_experts[:, :, None] == slots[None, None, :]
    dense_weights = jnp.sum(jnp.where(hits, route_weights[:, :, None], 0.0), axis=1)
    own_residual = lax.dynamic_slice_in_dim(
        residual[:seq_count], tp_index * quarter, quarter, 1
    ).astype(jnp.float32)
    mixture = own_residual
    for k in range(ep_size):
        here = pair_sum[k, :, :quarter]
        there = pair_sum[k, :, quarter:]
        here = here if k == 0 else swap_both(here, k, 0)
        there = swap_both(there, k, 2)
        expert_out = here.astype(jnp.float32) + there.astype(jnp.float32)
        mixture = mixture + dense_weights[:, k : k + 1] * expert_out
    return (mixture.astype(jnp.bfloat16), new_state)


def solution(mesh):
    in_specs = (
        P("ep", None),
        P("ep", "tp", None, None),
        P(None, "tp"),
        P(None, "tp"),
        P(None, "tp"),
        P(),
        P(None, "tp"),
        P("tp"),
        P(),
        P(None, "tp"),
        P("tp"),
        P("tp"),
        P("tp", None),
        P("ep", None),
        P("ep", None),
        P("ep", None, "tp"),
        P("ep", None, "tp"),
        P("ep", "tp", None),
    )
    out_specs = (P("ep", "tp"), P("ep", "tp", None, None))
    ep_size, tp_size = mesh.shape["ep"], mesh.shape["tp"]

    def local(*operands):
        seq_count, top_count = operands[13].shape
        capacity = max(2, (2 * seq_count * top_count + ep_size - 1) // ep_size)
        powers = ep_size & (ep_size - 1) == 0 and tp_size == 4
        if capacity >= seq_count and powers:
            return dense_local(*operands)
        return compact_local(*operands)

    return jax.shard_map(local, mesh=mesh, in_specs=in_specs, out_specs=out_specs, check_vma=False)
```

```python
import jax
import jax.numpy as jnp
from jax import lax
from jax.experimental import pallas as pl
from jax.sharding import PartitionSpec as P

NORM_EPS = 1e-05
GROUP_EPS = 0.00064
UNIT_EPS = 1e-06
CLAMP_LIMIT = 7.0
GLU_ALPHA = 1.702


def row_norm(values):
    return values * lax.rsqrt(jnp.mean(values * values, axis=-1, keepdims=True) + NORM_EPS)


def clamped_unit(gate_pre, up_pre):
    gated = jnp.minimum(gate_pre, CLAMP_LIMIT)
    linear = jnp.clip(up_pre, -CLAMP_LIMIT, CLAMP_LIMIT)
    return gated * jax.nn.sigmoid(GLU_ALPHA * gated) * (linear + 1.0)


def update_heads(head_state, recept, keys, values, decay_rate, rate_gate, head_gain):
    seq_count, head_count, head_size = head_state.shape[:3]

    def by_heads(operand):
        return operand.astype(jnp.float32).reshape(seq_count, head_count, head_size)

    recept_heads = by_heads(recept)
    key_heads = by_heads(keys)
    value_heads = by_heads(values)
    decay_heads = by_heads(decay_rate)
    rate_heads = by_heads(rate_gate)
    unit_key = key_heads * lax.rsqrt(
        jnp.sum(key_heads * key_heads, axis=-1, keepdims=True) + UNIT_EPS
    )
    highest = lax.Precision.HIGHEST
    state_unit = jnp.einsum("shvk,shk->shv", head_state, unit_key, precision=highest)
    new_state = (
        head_state * decay_heads[:, :, None, :]
        - state_unit[..., None] * (unit_key * rate_heads)[:, :, None, :]
        + value_heads[..., None] * (key_heads * rate_heads)[:, :, None, :]
    )
    head_out = jnp.einsum("shvk,shk->shv", new_state, recept_heads, precision=highest)
    centre = jnp.mean(head_out, axis=-1, keepdims=True)
    spread = jnp.mean(jnp.square(head_out - centre), axis=-1, keepdims=True)
    normed_heads = (head_out - centre) * lax.rsqrt(spread + GROUP_EPS)
    mixed = (normed_heads.reshape(seq_count, -1) * head_gain).astype(jnp.bfloat16)
    return (new_state, mixed)


def attention(
    tokens,
    head_state,
    recept_weight,
    key_weight,
    value_weight,
    decay_down_factor,
    decay_up_factor,
    decay_base,
    rate_down_factor,
    rate_up_factor,
    rate_base,
    head_gain,
):
    tokens_float = tokens.astype(jnp.float32)
    normed = row_norm(tokens_float).astype(jnp.bfloat16)
    recept = jnp.dot(normed, recept_weight, preferred_element_type=jnp.float32).astype(jnp.bfloat16)
    keys = jnp.dot(normed, key_weight, preferred_element_type=jnp.float32).astype(jnp.bfloat16)
    values = jnp.dot(normed, value_weight, preferred_element_type=jnp.float32).astype(jnp.bfloat16)
    decay_low = jnp.tanh(
        jnp.dot(normed, decay_down_factor, preferred_element_type=jnp.float32)
    ).astype(jnp.bfloat16)
    rate_low = jnp.dot(normed, rate_down_factor, preferred_element_type=jnp.float32).astype(
        jnp.bfloat16
    )
    decay_pre = decay_base + jnp.dot(decay_low, decay_up_factor, preferred_element_type=jnp.float32)
    decay_rate = jnp.exp(-jnp.exp(-jax.nn.softplus(-decay_pre) - 0.5))
    rate_gate = jax.nn.sigmoid(
        rate_base + jnp.dot(rate_low, rate_up_factor, preferred_element_type=jnp.float32)
    )
    new_state, mixed = update_heads(
        head_state, recept, keys, values, decay_rate, rate_gate, head_gain
    )
    return (new_state, mixed)


def compact_local(
    tokens,
    head_state,
    recept_weight,
    key_weight,
    value_weight,
    decay_down_factor,
    decay_up_factor,
    decay_base,
    rate_down_factor,
    rate_up_factor,
    rate_base,
    head_gain,
    out_weight,
    route_experts,
    route_weights,
    expert_gate,
    expert_up,
    expert_down,
):
    tokens_float = tokens.astype(jnp.float32)
    new_state, mixed = attention(
        tokens,
        head_state,
        recept_weight,
        key_weight,
        value_weight,
        decay_down_factor,
        decay_up_factor,
        decay_base,
        rate_down_factor,
        rate_up_factor,
        rate_base,
        head_gain,
    )
    partial_value = jnp.dot(mixed, out_weight, preferred_element_type=jnp.float32).astype(
        jnp.bfloat16
    )
    partial_value = lax.optimization_barrier(partial_value).astype(jnp.float32)
    summed = lax.psum(partial_value.astype(jnp.bfloat16), "tp").astype(jnp.float32)
    residual = (tokens_float + summed).astype(jnp.bfloat16)
    expert_input = row_norm(residual.astype(jnp.float32)).astype(jnp.bfloat16)
    seq_count, top_count = route_experts.shape
    expert_count = lax.axis_size("ep")
    capacity = max(2, (2 * seq_count * top_count + expert_count - 1) // expert_count)
    column_count = expert_input.shape[1] // lax.axis_size("tp")
    column_start = lax.axis_index("tp") * column_count
    flat_routes = route_experts.reshape(-1)
    onehot = (flat_routes[:, None] == jnp.arange(expert_count, dtype=jnp.int32)[None, :]).astype(
        jnp.int32
    )
    earlier = jnp.cumsum(onehot, axis=0) - onehot
    target = flat_routes * capacity + jnp.sum(earlier * onehot, axis=1)
    slot_ids = jnp.arange(expert_count * capacity, dtype=jnp.int32)
    dispatch_map = jnp.any(
        slot_ids[:, None, None] == target.reshape(seq_count, top_count)[None], axis=-1
    )
    dispatch_map = dispatch_map.astype(jnp.bfloat16)
    outgoing = lax.dynamic_slice_in_dim(expert_input, column_start, column_count, 1)
    buffer = jnp.dot(dispatch_map, outgoing, preferred_element_type=jnp.float32).astype(
        jnp.bfloat16
    )
    buffer = buffer.reshape(expert_count, capacity, outgoing.shape[1])
    slot_rows = lax.all_gather(
        lax.all_to_all(buffer, "ep", split_axis=0, concat_axis=0, tiled=True),
        "tp",
        axis=2,
        tiled=True,
    )
    source_count, slot_count, model_width = slot_rows.shape
    flat_rows = slot_rows.reshape(-1, model_width)
    gate_pre = jnp.dot(flat_rows, expert_gate[0], preferred_element_type=jnp.float32)
    up_pre = jnp.dot(flat_rows, expert_up[0], preferred_element_type=jnp.float32)
    activated = clamped_unit(gate_pre, up_pre).astype(jnp.bfloat16)
    part_out = jnp.dot(activated, expert_down[0], preferred_element_type=jnp.float32).astype(
        jnp.bfloat16
    )
    part_out = lax.optimization_barrier(part_out).astype(jnp.float32)
    part_out = part_out.reshape(source_count, slot_count, model_width)
    shares = lax.psum_scatter(part_out.astype(jnp.bfloat16), "tp", scatter_dimension=2, tiled=True)
    returned = lax.all_to_all(shares, "ep", split_axis=0, concat_axis=0, tiled=True)
    picked = returned.reshape(expert_count * capacity, column_count)[target]
    picked = picked.reshape(seq_count, top_count, column_count).astype(jnp.float32)
    mixture = jnp.sum(route_weights[:, :, None] * picked, axis=1)
    own_residual = lax.dynamic_slice_in_dim(residual, column_start, column_count, 1).astype(
        jnp.float32
    )
    layer_out = (own_residual + mixture).astype(jnp.bfloat16)
    return (layer_out, new_state)


def swap(operand, axis, offset):
    size = lax.axis_size(axis)
    return lax.ppermute(operand, axis, [(i, i ^ offset) for i in range(size)])


def swap_both(operand, ep_offset, tp_offset):
    ep_size, tp_size = lax.axis_size("ep"), lax.axis_size("tp")
    pairs = [
        (e * tp_size + t, (e ^ ep_offset) * tp_size + (t ^ tp_offset))
        for e in range(ep_size)
        for t in range(tp_size)
    ]
    return lax.ppermute(operand, ("ep", "tp"), pairs)


def project_kernel(
    tokens,
    recept_weight,
    key_weight,
    value_weight,
    decay_down,
    decay_up,
    decay_base,
    rate_down,
    rate_up,
    rate_base,
    query_out,
    read_out,
    value_out,
    cross_out,
    decay_out,
    key_rate_out,
):
    def dot(left, right):
        return jnp.dot(left, right, preferred_element_type=jnp.float32)

    normed = row_norm(tokens[...].astype(jnp.float32)).astype(jnp.bfloat16)
    recept = dot(normed, recept_weight[...]).astype(jnp.bfloat16).astype(jnp.float32)
    keys = dot(normed, key_weight[...]).astype(jnp.bfloat16).astype(jnp.float32)
    values = dot(normed, value_weight[...]).astype(jnp.bfloat16).astype(jnp.float32)
    decay_low = jnp.tanh(dot(normed, decay_down[...])).astype(jnp.bfloat16)
    rate_low = dot(normed, rate_down[...]).astype(jnp.bfloat16)
    decay_pre = decay_base[...] + dot(decay_low, decay_up[...])
    decay = jnp.exp(-jnp.exp(-jax.nn.softplus(-decay_pre) - 0.5))
    rate = jax.nn.sigmoid(rate_base[...] + dot(rate_low, rate_up[...]))
    key_rate = keys * rate
    read = decay * recept
    cross = key_rate * recept
    squares = keys * keys
    decay_out[...] = decay
    key_rate_out[...] = key_rate
    head_count, _, size = query_out.shape
    for h in range(head_count):
        own = slice(h * size, (h + 1) * size)
        scale = lax.rsqrt(jnp.sum(squares[:, own], axis=-1, keepdims=True) + UNIT_EPS)
        query_out[h] = keys[:, own] * (scale * scale)
        read_out[h] = read[:, own]
        value_out[h] = values[:, own]
        total = jnp.sum(cross[:, own], axis=-1, keepdims=True)
        cross_out[h] = jnp.broadcast_to(total, cross_out.shape[1:])


def state_kernel(state, query, read, value, cross, gain, mixed_out, write_out):
    head_count, size = state.shape[1], state.shape[2]
    rows = lax.broadcasted_iota(jnp.int32, (size, size), 0)
    columns = lax.broadcasted_iota(jnp.int32, (size, size), 1)
    diagonal = (rows == columns)[None]

    def times(own, vectors):
        sums = jnp.sum(own * vectors[:, None, :], axis=-1, keepdims=True)
        return jnp.sum(jnp.where(diagonal, sums, 0.0), axis=1)

    mixed, writes = [], []
    for h in range(head_count):
        own = state[:, h]
        write = value[h] - times(own, query[h])
        out = times(own, read[h]) + write * cross[h]
        centred = out - jnp.mean(out, axis=-1, keepdims=True)
        spread = jnp.mean(centred * centred, axis=-1, keepdims=True)
        mixed.append(centred * lax.rsqrt(spread + GROUP_EPS))
        writes.append(write)
    mixed_out[...] = jnp.concatenate(mixed, axis=1) * gain[...]
    write_out[...] = jnp.concatenate(writes, axis=1)


ROWS = 8


def read_state(head_state, parts, head_gain, first, count):
    head_count, size = head_state.shape[1:3]
    offset = first // ROWS
    part = pl.BlockSpec((head_count, ROWS, size), lambda i: (0, i + offset, 0))
    row = pl.BlockSpec((ROWS, head_count * size), lambda i: (i, 0))
    shape = jax.ShapeDtypeStruct((count, head_count * size), jnp.float32)
    return pl.pallas_call(
        state_kernel,
        grid=(count // ROWS,),
        in_specs=[
            pl.BlockSpec((ROWS, head_count, size, size), lambda i: (i + offset, 0, 0, 0)),
            part,
            part,
            part,
            part,
            pl.BlockSpec((1, head_count * size), lambda i: (0, 0)),
        ],
        out_specs=[row, row],
        out_shape=[shape, shape],
        name="read_state",
    )(head_state, *parts, head_gain[None])


def dense_local(
    tokens,
    head_state,
    recept_weight,
    key_weight,
    value_weight,
    decay_down_factor,
    decay_up_factor,
    decay_base,
    rate_down_factor,
    rate_up_factor,
    rate_base,
    head_gain,
    out_weight,
    route_experts,
    route_weights,
    expert_gate,
    expert_up,
    expert_down,
):
    ep_size, tp_size = lax.axis_size("ep"), lax.axis_size("tp")
    ep_index, tp_index = lax.axis_index("ep"), lax.axis_index("tp")
    seq_count, model_width = tokens.shape
    head_count, head_size = head_state.shape[1:3]
    half = model_width // 2
    quarter = model_width // tp_size
    odd = tp_index % 2 == 1
    steps = []
    step = ep_size // 2
    while step > 1:
        steps.append(step)
        step //= 2
    order = [0]
    for step in steps:
        order = order + [k + step for k in order]

    experts = jnp.arange(ep_size, dtype=jnp.int32)
    hits = route_experts[:, :, None] == experts[None, None, :]
    weights = jnp.sum(jnp.where(hits, route_weights[:, :, None], 0.0), axis=1)
    upper = lax.reduce_precision(weights, 8, 7)
    lower = weights - upper
    weight_columns = jnp.concatenate([upper, lower], axis=1).astype(jnp.bfloat16)
    weight_columns = jnp.pad(weight_columns, ((0, 0), (0, 128 - 2 * ep_size)))

    own_half = jnp.where(odd, tokens[:, half:], tokens[:, :half])
    sent = jnp.concatenate([own_half, weight_columns], axis=1)
    weight_far = swap(out_weight, "tp", 2)
    sent = jnp.concatenate([sent, swap(sent, "ep", steps[0])], axis=0)

    width = head_count * head_size
    part = jax.ShapeDtypeStruct((head_count, seq_count, head_size), jnp.float32)
    flat = jax.ShapeDtypeStruct((seq_count, width), jnp.float32)
    *parts, decay, key_rate = pl.pallas_call(
        project_kernel, out_shape=[part, part, part, part, flat, flat], name="project"
    )(
        tokens,
        recept_weight,
        key_weight,
        value_weight,
        decay_down_factor,
        decay_up_factor,
        decay_base[None],
        rate_down_factor,
        rate_up_factor,
        rate_base[None],
    )
    sent, parts = lax.optimization_barrier((sent, parts))
    for step in steps[1:]:
        sent = jnp.concatenate([sent, swap(sent, "ep", step)], axis=0)
    first = seq_count // 2
    mixed_a, write_a = read_state(head_state, parts, head_gain, 0, first)
    sent, parts, mixed_a = lax.optimization_barrier((sent, parts, mixed_a))
    sent = jnp.concatenate([sent, swap(sent, "ep", 1)], axis=0)
    mixed_b, write_b = read_state(head_state, parts, head_gain, first, seq_count - first)
    mixed = jnp.concatenate([mixed_a, mixed_b], axis=0).astype(jnp.bfloat16)
    write = jnp.concatenate([write_a, write_b], axis=0)

    near = [mixed] + [swap(mixed, "ep", k) for k in order[1:]]
    near = jnp.concatenate(near, axis=0)
    across = swap_both(near, 1, 2)
    far = swap_both(near, 0, 2)
    beside = swap_both(near, 1, 0)
    mixed_pair = jnp.concatenate(
        [jnp.concatenate([near, beside], axis=0), jnp.concatenate([far, across], axis=0)], axis=1
    )
    weight_pair = jnp.concatenate([out_weight, weight_far], axis=0)
    partner_weight = swap(weight_pair, "tp", 1)
    partner_sent = swap(sent[:, :half], "tp", 1)
    partner_mixed = swap(mixed_pair, "tp", 1)
    kept_half = sent[:, :half]
    low = jnp.where(odd, partner_sent, kept_half)
    high = jnp.where(odd, kept_half, partner_sent)
    tokens_all = jnp.concatenate([low, high], axis=1)
    own_weights = sent[:, half : half + 2 * ep_size].astype(jnp.float32)
    own_weights = own_weights[:, :ep_size] + own_weights[:, ep_size:]
    own_weights = jnp.sum(
        jnp.where(experts[None, :] == ep_index, own_weights, 0.0), axis=1, keepdims=True
    )
    projected = jnp.dot(mixed_pair, weight_pair, preferred_element_type=jnp.float32)
    projected += jnp.dot(partner_mixed, partner_weight, preferred_element_type=jnp.float32)
    residual = (tokens_all.astype(jnp.float32) + projected).astype(jnp.bfloat16)
    expert_input = row_norm(residual.astype(jnp.float32)).astype(jnp.bfloat16)

    by_key = (seq_count, head_count, 1, head_size)
    new_state = head_state * decay.reshape(by_key) + write.reshape(
        seq_count, head_count, head_size, 1
    ) * key_rate.reshape(by_key)

    gate_pre = jnp.dot(expert_input, expert_gate[0], preferred_element_type=jnp.float32)
    up_pre = jnp.dot(expert_input, expert_up[0], preferred_element_type=jnp.float32)
    activated = clamped_unit(gate_pre, up_pre).astype(jnp.bfloat16)

    def down(slots):
        pieces = [
            lax.dynamic_slice_in_dim(expert_down[0], (tp_index ^ j) * quarter, quarter, 1)
            for j in slots
        ]
        out = jnp.dot(
            activated, jnp.concatenate(pieces, axis=1), preferred_element_type=jnp.float32
        )
        return out * own_weights

    partner_out = swap(down((1, 3)).astype(jnp.bfloat16), "tp", 1)
    pair_sum = down((0, 2)) + partner_out.astype(jnp.float32)
    kept = pair_sum.astype(jnp.bfloat16)
    middle = ep_size // 2 * seq_count
    across = swap_both(kept[middle:, quarter:], 1, 2)
    far = swap_both(kept[:middle, quarter:], 0, 2)
    beside = swap_both(kept[middle:, :quarter], 1, 0)
    total = pair_sum[:middle, :quarter] + across.astype(jnp.float32)
    total = total + far.astype(jnp.float32) + beside.astype(jnp.float32)
    mixture = lax.dynamic_slice_in_dim(
        residual[:seq_count], tp_index * quarter, quarter, 1
    ).astype(jnp.float32)
    mixture = mixture + total[:seq_count]
    total = total.astype(jnp.bfloat16)
    for place, k in enumerate(order):
        if k:
            piece = total[place * seq_count : (place + 1) * seq_count]
            mixture = mixture + swap(piece, "ep", k).astype(jnp.float32)
    return (mixture.astype(jnp.bfloat16), new_state)


def solution(mesh):
    in_specs = (
        P("ep", None),
        P("ep", "tp", None, None),
        P(None, "tp"),
        P(None, "tp"),
        P(None, "tp"),
        P(),
        P(None, "tp"),
        P("tp"),
        P(),
        P(None, "tp"),
        P("tp"),
        P("tp"),
        P("tp", None),
        P("ep", None),
        P("ep", None),
        P("ep", None, "tp"),
        P("ep", None, "tp"),
        P("ep", "tp", None),
    )
    out_specs = (P("ep", "tp"), P("ep", "tp", None, None))
    ep_size, tp_size = mesh.shape["ep"], mesh.shape["tp"]

    def local(*operands):
        seq_count, top_count = operands[13].shape
        capacity = max(2, (2 * seq_count * top_count + ep_size - 1) // ep_size)
        powers = ep_size & (ep_size - 1) == 0 and 4 <= ep_size <= 64 and tp_size == 4
        powers = powers and seq_count % (2 * ROWS) == 0
        if capacity >= seq_count and powers:
            return dense_local(*operands)
        return compact_local(*operands)

    return jax.shard_map(local, mesh=mesh, in_specs=in_specs, out_specs=out_specs, check_vma=False)
```

```python
import jax
import jax.numpy as jnp
from jax import lax
from jax.experimental import pallas as pl
from jax.experimental.pallas import tpu as pltpu
from jax.sharding import PartitionSpec as P

NORM_EPS = 1e-05
GROUP_EPS = 0.00064
UNIT_EPS = 1e-06
CLAMP_LIMIT = 7.0
GLU_ALPHA = 1.702


def row_norm(values):
    return values * lax.rsqrt(jnp.mean(values * values, axis=-1, keepdims=True) + NORM_EPS)


def clamped_unit(gate_pre, up_pre):
    gated = jnp.minimum(gate_pre, CLAMP_LIMIT)
    linear = jnp.clip(up_pre, -CLAMP_LIMIT, CLAMP_LIMIT)
    return gated * jax.nn.sigmoid(GLU_ALPHA * gated) * (linear + 1.0)


def update_heads(head_state, recept, keys, values, decay_rate, rate_gate, head_gain):
    seq_count, head_count, head_size = head_state.shape[:3]

    def by_heads(operand):
        return operand.astype(jnp.float32).reshape(seq_count, head_count, head_size)

    recept_heads = by_heads(recept)
    key_heads = by_heads(keys)
    value_heads = by_heads(values)
    decay_heads = by_heads(decay_rate)
    rate_heads = by_heads(rate_gate)
    unit_key = key_heads * lax.rsqrt(
        jnp.sum(key_heads * key_heads, axis=-1, keepdims=True) + UNIT_EPS
    )
    highest = lax.Precision.HIGHEST
    state_unit = jnp.einsum("shvk,shk->shv", head_state, unit_key, precision=highest)
    new_state = (
        head_state * decay_heads[:, :, None, :]
        - state_unit[..., None] * (unit_key * rate_heads)[:, :, None, :]
        + value_heads[..., None] * (key_heads * rate_heads)[:, :, None, :]
    )
    head_out = jnp.einsum("shvk,shk->shv", new_state, recept_heads, precision=highest)
    centre = jnp.mean(head_out, axis=-1, keepdims=True)
    spread = jnp.mean(jnp.square(head_out - centre), axis=-1, keepdims=True)
    normed_heads = (head_out - centre) * lax.rsqrt(spread + GROUP_EPS)
    mixed = (normed_heads.reshape(seq_count, -1) * head_gain).astype(jnp.bfloat16)
    return (new_state, mixed)


def attention(
    tokens,
    head_state,
    recept_weight,
    key_weight,
    value_weight,
    decay_down_factor,
    decay_up_factor,
    decay_base,
    rate_down_factor,
    rate_up_factor,
    rate_base,
    head_gain,
):
    tokens_float = tokens.astype(jnp.float32)
    normed = row_norm(tokens_float).astype(jnp.bfloat16)
    recept = jnp.dot(normed, recept_weight, preferred_element_type=jnp.float32).astype(jnp.bfloat16)
    keys = jnp.dot(normed, key_weight, preferred_element_type=jnp.float32).astype(jnp.bfloat16)
    values = jnp.dot(normed, value_weight, preferred_element_type=jnp.float32).astype(jnp.bfloat16)
    decay_low = jnp.tanh(
        jnp.dot(normed, decay_down_factor, preferred_element_type=jnp.float32)
    ).astype(jnp.bfloat16)
    rate_low = jnp.dot(normed, rate_down_factor, preferred_element_type=jnp.float32).astype(
        jnp.bfloat16
    )
    decay_pre = decay_base + jnp.dot(decay_low, decay_up_factor, preferred_element_type=jnp.float32)
    decay_rate = jnp.exp(-jnp.exp(-jax.nn.softplus(-decay_pre) - 0.5))
    rate_gate = jax.nn.sigmoid(
        rate_base + jnp.dot(rate_low, rate_up_factor, preferred_element_type=jnp.float32)
    )
    new_state, mixed = update_heads(
        head_state, recept, keys, values, decay_rate, rate_gate, head_gain
    )
    return (new_state, mixed)


def compact_local(
    tokens,
    head_state,
    recept_weight,
    key_weight,
    value_weight,
    decay_down_factor,
    decay_up_factor,
    decay_base,
    rate_down_factor,
    rate_up_factor,
    rate_base,
    head_gain,
    out_weight,
    route_experts,
    route_weights,
    expert_gate,
    expert_up,
    expert_down,
):
    tokens_float = tokens.astype(jnp.float32)
    new_state, mixed = attention(
        tokens,
        head_state,
        recept_weight,
        key_weight,
        value_weight,
        decay_down_factor,
        decay_up_factor,
        decay_base,
        rate_down_factor,
        rate_up_factor,
        rate_base,
        head_gain,
    )
    partial_value = jnp.dot(mixed, out_weight, preferred_element_type=jnp.float32).astype(
        jnp.bfloat16
    )
    partial_value = lax.optimization_barrier(partial_value).astype(jnp.float32)
    summed = lax.psum(partial_value.astype(jnp.bfloat16), "tp").astype(jnp.float32)
    residual = (tokens_float + summed).astype(jnp.bfloat16)
    expert_input = row_norm(residual.astype(jnp.float32)).astype(jnp.bfloat16)
    seq_count, top_count = route_experts.shape
    expert_count = lax.axis_size("ep")
    capacity = max(2, (2 * seq_count * top_count + expert_count - 1) // expert_count)
    column_count = expert_input.shape[1] // lax.axis_size("tp")
    column_start = lax.axis_index("tp") * column_count
    flat_routes = route_experts.reshape(-1)
    onehot = (flat_routes[:, None] == jnp.arange(expert_count, dtype=jnp.int32)[None, :]).astype(
        jnp.int32
    )
    earlier = jnp.cumsum(onehot, axis=0) - onehot
    target = flat_routes * capacity + jnp.sum(earlier * onehot, axis=1)
    slot_ids = jnp.arange(expert_count * capacity, dtype=jnp.int32)
    dispatch_map = jnp.any(
        slot_ids[:, None, None] == target.reshape(seq_count, top_count)[None], axis=-1
    )
    dispatch_map = dispatch_map.astype(jnp.bfloat16)
    outgoing = lax.dynamic_slice_in_dim(expert_input, column_start, column_count, 1)
    buffer = jnp.dot(dispatch_map, outgoing, preferred_element_type=jnp.float32).astype(
        jnp.bfloat16
    )
    buffer = buffer.reshape(expert_count, capacity, outgoing.shape[1])
    slot_rows = lax.all_gather(
        lax.all_to_all(buffer, "ep", split_axis=0, concat_axis=0, tiled=True),
        "tp",
        axis=2,
        tiled=True,
    )
    source_count, slot_count, model_width = slot_rows.shape
    flat_rows = slot_rows.reshape(-1, model_width)
    gate_pre = jnp.dot(flat_rows, expert_gate[0], preferred_element_type=jnp.float32)
    up_pre = jnp.dot(flat_rows, expert_up[0], preferred_element_type=jnp.float32)
    activated = clamped_unit(gate_pre, up_pre).astype(jnp.bfloat16)
    part_out = jnp.dot(activated, expert_down[0], preferred_element_type=jnp.float32).astype(
        jnp.bfloat16
    )
    part_out = lax.optimization_barrier(part_out).astype(jnp.float32)
    part_out = part_out.reshape(source_count, slot_count, model_width)
    shares = lax.psum_scatter(part_out.astype(jnp.bfloat16), "tp", scatter_dimension=2, tiled=True)
    returned = lax.all_to_all(shares, "ep", split_axis=0, concat_axis=0, tiled=True)
    picked = returned.reshape(expert_count * capacity, column_count)[target]
    picked = picked.reshape(seq_count, top_count, column_count).astype(jnp.float32)
    mixture = jnp.sum(route_weights[:, :, None] * picked, axis=1)
    own_residual = lax.dynamic_slice_in_dim(residual, column_start, column_count, 1).astype(
        jnp.float32
    )
    layer_out = (own_residual + mixture).astype(jnp.bfloat16)
    return (layer_out, new_state)


def swap(operand, axis, offset):
    size = lax.axis_size(axis)
    return lax.ppermute(operand, axis, [(i, i ^ offset) for i in range(size)])


def swap_both(operand, ep_offset, tp_offset):
    ep_size, tp_size = lax.axis_size("ep"), lax.axis_size("tp")
    pairs = [
        (e * tp_size + t, (e ^ ep_offset) * tp_size + (t ^ tp_offset))
        for e in range(ep_size)
        for t in range(tp_size)
    ]
    return lax.ppermute(operand, ("ep", "tp"), pairs)


def project_kernel(
    tokens,
    recept_weight,
    key_weight,
    value_weight,
    decay_down,
    decay_up,
    decay_base,
    rate_down,
    rate_up,
    rate_base,
    query_out,
    read_out,
    value_out,
    cross_out,
    decay_out,
    key_rate_out,
):
    def dot(left, right):
        return jnp.dot(left, right, preferred_element_type=jnp.float32)

    def dot_rows(left, right):
        return lax.dot_general(
            left, right, (((1,), (1,)), ((), ())), preferred_element_type=jnp.float32
        )

    normed = row_norm(tokens[...].astype(jnp.float32)).astype(jnp.bfloat16)
    recept = dot(normed, recept_weight[...]).astype(jnp.bfloat16).astype(jnp.float32)
    keys = dot(normed, key_weight[...]).astype(jnp.bfloat16).astype(jnp.float32)
    values = dot(normed, value_weight[...]).astype(jnp.bfloat16).astype(jnp.float32)
    decay_low = jnp.tanh(dot_rows(normed, decay_down[...])).astype(jnp.bfloat16)
    rate_low = dot_rows(normed, rate_down[...]).astype(jnp.bfloat16)
    decay_pre = decay_base[...] + dot(decay_low, decay_up[...])
    decay = jnp.exp(-jnp.exp(-jax.nn.softplus(-decay_pre) - 0.5))
    rate = jax.nn.sigmoid(rate_base[...] + dot(rate_low, rate_up[...]))
    key_rate = keys * rate
    read = decay * recept
    cross = key_rate * recept
    squares = keys * keys
    decay_out[...] = decay
    key_rate_out[...] = key_rate
    head_count, _, size = query_out.shape
    for h in range(head_count):
        own = slice(h * size, (h + 1) * size)
        scale = lax.rsqrt(jnp.sum(squares[:, own], axis=-1, keepdims=True) + UNIT_EPS)
        query_out[h] = keys[:, own] * (scale * scale)
        read_out[h] = read[:, own]
        value_out[h] = values[:, own]
        total = jnp.sum(cross[:, own], axis=-1, keepdims=True)
        cross_out[h] = jnp.broadcast_to(total, cross_out.shape[1:])


def state_kernel(state, query, read, value, cross, gain, mixed_out, write_out, mixed_rows):
    head_count, size = state.shape[1], state.shape[2]
    rows = lax.broadcasted_iota(jnp.int32, (size, size), 0)
    columns = lax.broadcasted_iota(jnp.int32, (size, size), 1)
    diagonal = (rows == columns)[None]

    def times(own, vectors):
        sums = jnp.sum(own * vectors[:, None, :], axis=-1, keepdims=True)
        return jnp.sum(jnp.where(diagonal, sums, 0.0), axis=1)

    mixed, writes = [], []
    for h in range(head_count):
        own = state[:, h]
        write = value[h] - times(own, query[h])
        out = times(own, read[h]) + write * cross[h]
        centred = out - jnp.mean(out, axis=-1, keepdims=True)
        spread = jnp.mean(centred * centred, axis=-1, keepdims=True)
        mixed.append(centred * lax.rsqrt(spread + GROUP_EPS))
        writes.append(write)
    step = pl.program_id(0)
    mixed_rows[pl.ds(step * ROWS, ROWS), :] = jnp.concatenate(mixed, axis=1) * gain[...]

    @pl.when(step == pl.num_programs(0) - 1)
    def _():
        mixed_out[...] = mixed_rows[...].astype(jnp.bfloat16)

    write_out[...] = jnp.concatenate(writes, axis=1)


ROWS = 16


def read_state(head_state, parts, head_gain):
    seq_count, head_count, size = head_state.shape[:3]
    width = head_count * size
    part = pl.BlockSpec((head_count, ROWS, size), lambda i: (0, i, 0))
    return pl.pallas_call(
        state_kernel,
        grid=(seq_count // ROWS,),
        in_specs=[
            pl.BlockSpec((ROWS, head_count, size, size), lambda i: (i, 0, 0, 0)),
            part,
            part,
            part,
            part,
            pl.BlockSpec((1, width), lambda i: (0, 0)),
        ],
        out_specs=[
            pl.BlockSpec((seq_count, width), lambda i: (0, 0)),
            pl.BlockSpec((ROWS, width), lambda i: (i, 0)),
        ],
        out_shape=[
            jax.ShapeDtypeStruct((seq_count, width), jnp.bfloat16),
            jax.ShapeDtypeStruct((seq_count, width), jnp.float32),
        ],
        scratch_shapes=[pltpu.VMEM((seq_count, width), jnp.float32)],
        name="read_state",
    )(head_state, *parts, head_gain[None])


def dense_local(
    tokens,
    head_state,
    recept_weight,
    key_weight,
    value_weight,
    decay_down_factor,
    decay_up_factor,
    decay_base,
    rate_down_factor,
    rate_up_factor,
    rate_base,
    head_gain,
    out_weight,
    route_experts,
    route_weights,
    expert_gate,
    expert_up,
    expert_down,
):
    ep_size, tp_size = lax.axis_size("ep"), lax.axis_size("tp")
    ep_index, tp_index = lax.axis_index("ep"), lax.axis_index("tp")
    seq_count, model_width = tokens.shape
    head_count, head_size = head_state.shape[1:3]
    half = model_width // 2
    quarter = model_width // tp_size
    odd = tp_index % 2 == 1
    steps = []
    step = ep_size // 2
    while step > 1:
        steps.append(step)
        step //= 2
    order = [0]
    for step in steps:
        order = order + [k + step for k in order]

    experts = jnp.arange(ep_size, dtype=jnp.int32)
    hits = route_experts[:, :, None] == experts[None, None, :]
    weights = jnp.sum(jnp.where(hits, route_weights[:, :, None], 0.0), axis=1)
    upper = lax.reduce_precision(weights, 8, 7)
    lower = weights - upper
    weight_columns = jnp.concatenate([upper, lower], axis=1).astype(jnp.bfloat16)
    weight_columns = jnp.pad(weight_columns, ((0, 0), (0, 128 - 2 * ep_size)))

    own_half = jnp.where(odd, tokens[:, half:], tokens[:, :half])
    sent = jnp.concatenate([own_half, weight_columns], axis=1)
    weight_far = swap(out_weight, "tp", 2)
    sent = jnp.concatenate([sent, swap(sent, "ep", steps[0])], axis=0)

    width = head_count * head_size
    part = jax.ShapeDtypeStruct((head_count, seq_count, head_size), jnp.float32)
    flat = jax.ShapeDtypeStruct((seq_count, width), jnp.float32)
    *parts, decay, key_rate = pl.pallas_call(
        project_kernel, out_shape=[part, part, part, part, flat, flat], name="project"
    )(
        tokens,
        recept_weight,
        key_weight,
        value_weight,
        decay_down_factor.T,
        decay_up_factor,
        decay_base[None],
        rate_down_factor.T,
        rate_up_factor,
        rate_base[None],
    )
    sent, parts = lax.optimization_barrier((sent, parts))
    for step in steps[1:]:
        sent = jnp.concatenate([sent, swap(sent, "ep", step)], axis=0)
    mixed, write = read_state(head_state, parts, head_gain)
    sent = jnp.concatenate([sent, swap(sent, "ep", 1)], axis=0)

    near = [mixed] + [swap(mixed, "ep", k) for k in order[1:]]
    near = jnp.concatenate(near, axis=0)
    across = swap_both(near, 1, 2)
    far = swap_both(near, 0, 2)
    beside = swap_both(near, 1, 0)
    mixed_pair = jnp.concatenate(
        [jnp.concatenate([near, beside], axis=0), jnp.concatenate([far, across], axis=0)], axis=1
    )
    weight_pair = jnp.concatenate([out_weight, weight_far], axis=0)
    partner_weight = swap(weight_pair, "tp", 1)
    partner_sent = swap(sent[:, :half], "tp", 1)
    partner_mixed = swap(mixed_pair, "tp", 1)
    kept_half = sent[:, :half]
    low = jnp.where(odd, partner_sent, kept_half)
    high = jnp.where(odd, kept_half, partner_sent)
    tokens_all = jnp.concatenate([low, high], axis=1)
    own_weights = sent[:, half : half + 2 * ep_size].astype(jnp.float32)
    own_weights = own_weights[:, :ep_size] + own_weights[:, ep_size:]
    own_weights = jnp.sum(
        jnp.where(experts[None, :] == ep_index, own_weights, 0.0), axis=1, keepdims=True
    )
    projected = jnp.dot(mixed_pair, weight_pair, preferred_element_type=jnp.float32)
    projected += jnp.dot(partner_mixed, partner_weight, preferred_element_type=jnp.float32)
    residual = (tokens_all.astype(jnp.float32) + projected).astype(jnp.bfloat16)
    expert_input = row_norm(residual.astype(jnp.float32)).astype(jnp.bfloat16)

    by_key = (seq_count, head_count, 1, head_size)
    new_state = head_state * decay.reshape(by_key) + write.reshape(
        seq_count, head_count, head_size, 1
    ) * key_rate.reshape(by_key)

    gate_pre = jnp.dot(expert_input, expert_gate[0], preferred_element_type=jnp.float32)
    up_pre = jnp.dot(expert_input, expert_up[0], preferred_element_type=jnp.float32)
    activated = clamped_unit(gate_pre, up_pre).astype(jnp.bfloat16)

    def down(slots):
        pieces = [
            lax.dynamic_slice_in_dim(expert_down[0], (tp_index ^ j) * quarter, quarter, 1)
            for j in slots
        ]
        out = jnp.dot(
            activated, jnp.concatenate(pieces, axis=1), preferred_element_type=jnp.float32
        )
        return out * own_weights

    partner_out = swap(down((1, 3)).astype(jnp.bfloat16), "tp", 1)
    pair_sum = down((0, 2)) + partner_out.astype(jnp.float32)
    kept = pair_sum.astype(jnp.bfloat16)
    middle = ep_size // 2 * seq_count
    across = swap_both(kept[middle:, quarter:], 1, 2)
    far = swap_both(kept[:middle, quarter:], 0, 2)
    beside = swap_both(kept[middle:, :quarter], 1, 0)
    across, far, beside, new_state = lax.optimization_barrier((across, far, beside, new_state))
    total = pair_sum[:middle, :quarter] + across.astype(jnp.float32)
    total = total + far.astype(jnp.float32) + beside.astype(jnp.float32)
    mixture = lax.dynamic_slice_in_dim(
        residual[:seq_count], tp_index * quarter, quarter, 1
    ).astype(jnp.float32)
    mixture = mixture + total[:seq_count]
    total = total.astype(jnp.bfloat16)
    for place, k in enumerate(order):
        if k:
            piece = total[place * seq_count : (place + 1) * seq_count]
            mixture = mixture + swap(piece, "ep", k).astype(jnp.float32)
    return (mixture.astype(jnp.bfloat16), new_state)


def solution(mesh):
    in_specs = (
        P("ep", None),
        P("ep", "tp", None, None),
        P(None, "tp"),
        P(None, "tp"),
        P(None, "tp"),
        P(),
        P(None, "tp"),
        P("tp"),
        P(),
        P(None, "tp"),
        P("tp"),
        P("tp"),
        P("tp", None),
        P("ep", None),
        P("ep", None),
        P("ep", None, "tp"),
        P("ep", None, "tp"),
        P("ep", "tp", None),
    )
    out_specs = (P("ep", "tp"), P("ep", "tp", None, None))
    ep_size, tp_size = mesh.shape["ep"], mesh.shape["tp"]

    def local(*operands):
        seq_count, top_count = operands[13].shape
        capacity = max(2, (2 * seq_count * top_count + ep_size - 1) // ep_size)
        powers = ep_size & (ep_size - 1) == 0 and 4 <= ep_size <= 64 and tp_size == 4
        powers = powers and seq_count % ROWS == 0
        if capacity >= seq_count and powers:
            return dense_local(*operands)
        return compact_local(*operands)

    return jax.shard_map(local, mesh=mesh, in_specs=in_specs, out_specs=out_specs, check_vma=False)
```
